32 devices in a mesh: sp: 8 (over z, x), tp: 4 (over y, core).
Axes of the slice: x: 2, y: 2, z: 4, core: 2. Of those that a mesh axis runs over, the one named last changes fastest.
Arguments:
- layer_input: bfloat16 [1280, 4096], P('sp', 'tp'), may hold values from -24 to 24
- output_grad: bfloat16 [1280, 4096], P('sp', 'tp'), may hold values from -24 to 24
- query_weight: bfloat16 [4096, 2048], P(None, 'tp'), may hold values from -0.09375 to 0.09375
- key_weight: bfloat16 [4096, 1024], P(None, 'tp'), may hold values from -0.09375 to 0.09375
- value_weight: bfloat16 [4096, 1024], P(None, 'tp'), may hold values from -0.09375 to 0.09375
- out_weight: bfloat16 [2048, 4096], P('tp'), may hold values from -0.125 to 0.125
- sink_logit: float32 [16], P('tp'), may hold values from 3 to 7
Outputs:
- input_grad: bfloat16 [1280, 4096], P('sp', 'tp')
- query_weight_grad: float32 [4096, 2048], P('sp', 'tp')
- key_weight_grad: float32 [4096, 1024], P('sp', 'tp')
- value_weight_grad: float32 [4096, 1024], P('sp', 'tp')
- out_weight_grad: float32 [2048, 4096], P('tp', 'sp')
- sink_grad: float32 [16], P('tp')
The draws below stay inside these ranges and needn't reach their ends.
All inputs are finite; a program needn't handle non-finite values.
Results may differ from the reference program's by a relative error of at most 0.015.
Values may be sent and summed in bfloat16 or wider, within the bound.
No kernel may reach another device: no remote copies, remote signals or barrier semaphores. Data moves between devices by JAX's collectives and lax.ppermute only.
A program may use at most 192 MiB of HBM per device.

```python
import jax
import jax.numpy as jnp
from jax import lax

D = 4096
HEADS = 16
KV_HEADS = 8
HEAD = 128
WINDOW = 128
TOK_DEV = 160
TOKENS = 1280


def draw_layer_input(key, part):
    key_normal = jax.random.fold_in(key, 11)
    key_pairing = jax.random.fold_in(key, 12)
    normal_part = jnp.clip(jax.random.normal(key_normal, (TOKENS, D), jnp.float32), -4.0, 4.0)
    blocks = TOKENS // TOK_DEV
    pairing = jax.random.permutation(key_pairing, blocks)
    row_block = jnp.arange(TOKENS, dtype=jnp.int32) // TOK_DEV
    col_block = jnp.arange(D, dtype=jnp.int32) * blocks // D
    spiked = pairing[row_block][:, None] == col_block[None, :]
    values = normal_part * jnp.where(spiked, 3.0, 1.0)
    return values.astype(jnp.bfloat16)


def strengthened(entries, own_key, source, target, parts, factor):
    owner, partner = [(jnp.arange(entries.shape[axis_at]) // (entries.shape[axis_at] // parts)).reshape([-1 if axis == axis_at else 1 for axis in range(entries.ndim)]) for axis_at in (source, target)]
    chosen = jax.random.permutation(own_key, parts)[partner]
    strong = (owner == chosen) | (owner == (partner + parts // 2) % parts)
    return jnp.where(strong, factor * entries, entries)


def block_levels(stream_key, shape, cuts, smallest, largest):
    def one(dim, shards_of):
        draws = jax.random.uniform(jax.random.fold_in(jax.random.fold_in(stream_key, 6), dim), (shards_of,), jnp.float32, smallest / len(cuts), largest / len(cuts))
        return jnp.repeat(jnp.exp(draws), shape[dim] // shards_of).reshape((-1,) + (1,) * (len(shape) - dim - 1))

    level = one(*cuts[0])
    for cut in cuts[1:]:
        level = level * one(*cut)
    return level


def scatter_about(key, shape, deviation, limit, pieces=(), kind=jnp.bfloat16):
    entries = jax.random.normal(key, shape, jnp.float32) * deviation
    if len(pieces) > 0:
        entries = block_levels(key, shape, pieces, -0.22, 0.18) * entries
    return jnp.clip(entries, min=-limit, max=limit).astype(kind)


def bell_draw_with(stream_key, shape, deviation, bound, pieces, heavy, kind=jnp.bfloat16):
    entries = deviation * jax.random.normal(stream_key, shape, jnp.float32)
    if pieces:
        entries = entries * block_levels(stream_key, shape, pieces, -0.22, 0.18)
    return jnp.clip(strengthened(entries, jax.random.fold_in(stream_key, 3), *heavy), -bound, bound).astype(kind)


def setup_inputs(seed: int = 0) -> dict:
    key_list = jax.random.split(jax.random.key(seed), 8)
    return {
        "layer_input": draw_layer_input(jax.random.fold_in(key_list[7], 71), 0),
        "output_grad": bell_draw_with(key_list[1], (TOKENS, D), 4.0, 24.0, ((0, 8), (1, 4)), (0, 1, 8, 2.0)),
        "query_weight": scatter_about(key_list[2], (D, HEADS * HEAD), D ** -0.5, 0.09375, ((1, 4),)),
        "key_weight": scatter_about(key_list[3], (D, KV_HEADS * HEAD), D ** -0.5, 0.09375, ((1, 4),)),
        "value_weight": scatter_about(key_list[4], (D, KV_HEADS * HEAD), D ** -0.5, 0.09375, ((1, 4),)),
        "out_weight": scatter_about(key_list[5], (HEADS * HEAD, D), (HEADS * HEAD) ** -0.5, 0.125, ((0, 4),)),
        "sink_logit": jnp.clip(3.0 + 4.0 * jax.random.uniform(key_list[6], (HEADS,), jnp.float32) ** block_levels(key_list[6], (HEADS,), ((0, 4),), -0.2, 0.2), 3.0, 7.0),
    }


masked_score = -1e30


def reference(layer_input, output_grad, query_weight, key_weight, value_weight, out_weight, sink_logit):
    seq_len = layer_input.shape[0]
    group_size = HEADS // KV_HEADS
    scaling = HEAD ** -0.5
    block_count = seq_len // WINDOW
    queries = jnp.dot(layer_input, query_weight, preferred_element_type=jnp.float32).astype(jnp.bfloat16)
    queries = queries.reshape(seq_len, KV_HEADS, group_size, HEAD)
    key_rows = jnp.dot(layer_input, key_weight, preferred_element_type=jnp.float32).astype(jnp.bfloat16)
    key_rows = key_rows.reshape(seq_len, KV_HEADS, HEAD)
    value_rows = jnp.dot(layer_input, value_weight, preferred_element_type=jnp.float32).astype(jnp.bfloat16)
    value_rows = value_rows.reshape(seq_len, KV_HEADS, HEAD)
    out_rows_grad = jnp.dot(output_grad, out_weight.T, preferred_element_type=jnp.float32).astype(jnp.bfloat16)
    out_rows_grad = out_rows_grad.reshape(seq_len, KV_HEADS, group_size, HEAD)
    sink_column = sink_logit.astype(jnp.float32).reshape(KV_HEADS, group_size)[:, :, None]
    edge_three = ((WINDOW, WINDOW), (0, 0), (0, 0))
    edge_four = ((WINDOW, WINDOW), (0, 0), (0, 0), (0, 0))
    padded_keys = jnp.pad(key_rows, edge_three)
    padded_values = jnp.pad(value_rows, edge_three)

    def forward_block(block):
        offset = block * WINDOW
        query_block = lax.dynamic_slice_in_dim(queries, offset, WINDOW, 0).astype(jnp.float32)
        grad_block = lax.dynamic_slice_in_dim(out_rows_grad, offset, WINDOW, 0).astype(jnp.float32)
        key_band = lax.dynamic_slice_in_dim(padded_keys, offset, 3 * WINDOW, 0).astype(jnp.float32)
        value_band = lax.dynamic_slice_in_dim(padded_values, offset, 3 * WINDOW, 0).astype(jnp.float32)
        query_pos = offset + jnp.arange(WINDOW, dtype=jnp.int32)
        key_pos = offset - WINDOW + jnp.arange(3 * WINDOW, dtype=jnp.int32)
        in_window = (jnp.abs(query_pos[:, None] - key_pos[None, :]) <= WINDOW) & (key_pos[None, :] >= 0) & (key_pos[None, :] < seq_len)
        scores = jnp.einsum("qkgd,skd->kgqs", query_block, key_band) * scaling
        scores = jnp.where(in_window[None, None], scores, masked_score)
        row_max = jnp.maximum(jnp.max(scores, axis=-1), sink_column)
        row_total = jnp.sum(jnp.exp(scores - row_max[..., None]), axis=-1) + jnp.exp(sink_column - row_max)
        log_total = row_max + jnp.log(row_total)
        soft_weights = jnp.exp(scores - log_total[..., None])
        soft_rounded = soft_weights.astype(jnp.bfloat16)
        attended = jnp.einsum("kgqs,skd->qkgd", soft_rounded.astype(jnp.float32), value_band).astype(jnp.bfloat16)
        row_dots = jnp.sum(grad_block * attended.astype(jnp.float32), axis=-1)
        dots_moved = row_dots.transpose(1, 2, 0)
        prob_grads = jnp.einsum("qkgd,skd->kgqs", grad_block, value_band)
        score_grads = (soft_weights * (prob_grads - dots_moved[..., None])).astype(jnp.bfloat16)
        query_grads = (jnp.einsum("kgqs,skd->qkgd", score_grads.astype(jnp.float32), key_band) * scaling).astype(jnp.bfloat16)
        sink_part = -jnp.sum(jnp.exp(sink_column - log_total) * dots_moved, axis=-1)
        return attended, log_total, row_dots, query_grads, sink_part

    attended, log_total, row_dots, query_grads, sink_parts = lax.map(forward_block, jnp.arange(block_count, dtype=jnp.int32))
    attended = attended.reshape(seq_len, HEADS * HEAD)
    log_total = log_total.transpose(0, 3, 1, 2).reshape(seq_len, KV_HEADS, group_size)
    row_dots = row_dots.reshape(seq_len, KV_HEADS, group_size)
    query_grads = query_grads.reshape(seq_len, HEADS * HEAD)
    sink_grad = jnp.sum(sink_parts, axis=0).reshape(HEADS)
    padded_queries = jnp.pad(queries, edge_four)
    padded_out_grad = jnp.pad(out_rows_grad, edge_four)
    padded_totals = jnp.pad(log_total, edge_three)
    padded_dots = jnp.pad(row_dots, edge_three)

    def key_block(block):
        offset = block * WINDOW
        key_own = lax.dynamic_slice_in_dim(key_rows, offset, WINDOW, 0).astype(jnp.float32)
        value_own = lax.dynamic_slice_in_dim(value_rows, offset, WINDOW, 0).astype(jnp.float32)
        query_band = lax.dynamic_slice_in_dim(padded_queries, offset, 3 * WINDOW, 0).astype(jnp.float32)
        grad_band = lax.dynamic_slice_in_dim(padded_out_grad, offset, 3 * WINDOW, 0).astype(jnp.float32)
        total_band = lax.dynamic_slice_in_dim(padded_totals, offset, 3 * WINDOW, 0).transpose(1, 2, 0)
        dots_band = lax.dynamic_slice_in_dim(padded_dots, offset, 3 * WINDOW, 0).transpose(1, 2, 0)
        query_pos = offset - WINDOW + jnp.arange(3 * WINDOW, dtype=jnp.int32)
        key_pos = offset + jnp.arange(WINDOW, dtype=jnp.int32)
        in_window = (jnp.abs(query_pos[:, None] - key_pos[None, :]) <= WINDOW) & (query_pos[:, None] >= 0) & (query_pos[:, None] < seq_len)
        scores = jnp.einsum("qkgd,skd->kgqs", query_band, key_own) * scaling
        scores = jnp.where(in_window[None, None], scores, masked_score)
        soft_weights = jnp.exp(scores - total_band[..., None])
        soft_rounded = soft_weights.astype(jnp.bfloat16)
        prob_grads = jnp.einsum("qkgd,skd->kgqs", grad_band, value_own)
        score_grads = (soft_weights * (prob_grads - dots_band[..., None])).astype(jnp.bfloat16)
        key_grads = (jnp.einsum("kgqs,qkgd->skd", score_grads.astype(jnp.float32), query_band) * scaling).astype(jnp.bfloat16)
        value_grads = jnp.einsum("kgqs,qkgd->skd", soft_rounded.astype(jnp.float32), grad_band).astype(jnp.bfloat16)
        return key_grads, value_grads

    key_grads, value_grads = lax.map(key_block, jnp.arange(block_count, dtype=jnp.int32))
    key_grads = key_grads.reshape(seq_len, KV_HEADS * HEAD)
    value_grads = value_grads.reshape(seq_len, KV_HEADS * HEAD)
    input_grad = (jnp.dot(query_grads, query_weight.T, preferred_element_type=jnp.float32)
                  + jnp.dot(key_grads, key_weight.T, preferred_element_type=jnp.float32)
                  + jnp.dot(value_grads, value_weight.T, preferred_element_type=jnp.float32)).astype(jnp.bfloat16)
    query_weight_grad = jnp.dot(layer_input.T, query_grads, preferred_element_type=jnp.float32)
    key_weight_grad = jnp.dot(layer_input.T, key_grads, preferred_element_type=jnp.float32)
    value_weight_grad = jnp.dot(layer_input.T, value_grads, preferred_element_type=jnp.float32)
    out_weight_grad = jnp.dot(attended.T, output_grad, preferred_element_type=jnp.float32)
    return (input_grad, query_weight_grad, key_weight_grad, value_weight_grad, out_weight_grad, sink_grad)
```

```python
import functools

import jax
import jax.numpy as jnp
from jax import lax
from jax.experimental import pallas as pl
from jax.experimental.pallas import tpu as pltpu
from jax.sharding import PartitionSpec as P

HEADS = 16
KV_HEADS = 8
HEAD = 128
WINDOW = 128
GROUP = HEADS // KV_HEADS
SCALING = HEAD ** (-0.5)
MASKED = -1e30


bf16 = jnp.bfloat16
f32 = jnp.float32


def contract(left, right, ldim, rdim):
    return lax.dot_general(
        left, right, (((ldim,), (rdim,)), ((), ())), preferred_element_type=f32
    )


def whole_spec(array):
    rank = len(array.shape)
    return pl.BlockSpec(array.shape, lambda *_: (0,) * rank)


def cost(flops, moved):
    return pl.CostEstimate(flops=flops, transcendentals=0, bytes_accessed=moved)


def swap_tp(value, bit):
    return lax.ppermute(value, "tp", [(i, i ^ bit) for i in range(lax.axis_size("tp"))])


def ring_order(count):
    return list(range(0, count, 2)) + list(range(1, count, 2))[::-1]


def ring_shift(value, steps):
    count = lax.axis_size("sp")
    order = ring_order(count)
    pairs = [(order[p], order[(p + steps) % count]) for p in range(count)]
    return lax.ppermute(value, "sp", pairs)


def passed_along(value, steps):
    count = lax.axis_size("sp")
    first, last = max(0, -steps), min(count, count - steps)
    return lax.ppermute(value, "sp", [(i, i + steps) for i in range(first, last)])


def ring_gather(value):
    count = lax.axis_size("sp")
    blocks, forward, backward = [value], value, value
    for _ in range(count // 2 - 1):
        forward, backward = ring_shift(forward, 1), ring_shift(backward, -1)
        blocks += [forward, backward]
    half = value.shape[1] // 2
    blocks += [ring_shift(forward[:, :half], 1), ring_shift(backward[:, half:], -1)]
    return blocks


def project_first(order, xs, gs, weights):
    tok, feat = xs[0].shape
    qw, kw, vw, ow = weights
    qc, kc = qw.shape[1], kw.shape[1]

    def body(order_ref, xa, xb, ga, gb, qr, kr, vr, owr, q_out, kv_out, g_out):
        step = pl.program_id(0)

        def add(x, g, first):
            parts = [
                (q_out, slice(None), contract(x[...], qr[...], 1, 0)),
                (kv_out, slice(0, kc), contract(x[...], kr[...], 1, 0)),
                (kv_out, slice(kc, 2 * kc), contract(x[...], vr[...], 1, 0)),
                (g_out, slice(None), contract(g[...], owr[...], 1, 1)),
            ]
            for ref, cols, part in parts:
                ref[:, cols] = part if first else ref[:, cols] + part

        pl.when(step == 0)(lambda: add(xa, ga, True))
        pl.when(step == 1)(lambda: add(xb, gb, False))

    outs = [jax.ShapeDtypeStruct((tok, qc), f32), jax.ShapeDtypeStruct((tok, 2 * kc), f32),
            jax.ShapeDtypeStruct((tok, qc), f32)]
    rows = lambda cols: pl.BlockSpec((feat, cols), lambda t, o: (o[t], 0))
    return pl.pallas_call(
        body,
        grid_spec=pltpu.PrefetchScalarGridSpec(
            num_scalar_prefetch=1,
            grid=(2,),
            in_specs=[whole_spec(a) for a in (*xs, *gs)]
            + [rows(qc), rows(kc), rows(kc), pl.BlockSpec((qc, feat), lambda t, o: (0, o[t]))],
            out_specs=[whole_spec(o) for o in outs],
        ),
        out_shape=outs,
        cost_estimate=cost(4 * tok * feat * (2 * qc + 2 * kc), 4 * feat * (2 * qc + 2 * kc)),
        name="project_first",
    )(order, *xs, *gs, qw, kw, vw, ow)


def project_rows(order, xs, sums, weights):
    tok, feat = xs[0].shape
    qw, kw, vw = weights
    qc, kc = qw.shape[1], kw.shape[1]

    def body(order_ref, xa, xb, q_in, kv_in, qr, kr, vr, q_out, kv_out, q_acc, kv_acc):
        step = pl.program_id(0)

        def add(x, q_from, kv_from, q_to, kv_to):
            q_to[...] = (q_from[...] + contract(x[...], qr[...], 1, 0)).astype(q_to.dtype)
            for i, w in enumerate((kr, vr)):
                cols = slice(i * kc, (i + 1) * kc)
                kv_to[:, cols] = (
                    kv_from[:, cols] + contract(x[...], w[...], 1, 0)
                ).astype(kv_to.dtype)

        pl.when(step == 0)(lambda: add(xa, q_in, kv_in, q_acc, kv_acc))
        pl.when(step == 1)(lambda: add(xb, q_acc, kv_acc, q_out, kv_out))

    outs = [jax.ShapeDtypeStruct((tok, qc), bf16), jax.ShapeDtypeStruct((tok, 2 * kc), bf16)]
    rows = lambda cols: pl.BlockSpec((feat, cols), lambda t, o: (o[2 + t], 0))
    return pl.pallas_call(
        body,
        grid_spec=pltpu.PrefetchScalarGridSpec(
            num_scalar_prefetch=1,
            grid=(2,),
            in_specs=[whole_spec(a) for a in (*xs, *sums)] + [rows(qc), rows(kc), rows(kc)],
            out_specs=[whole_spec(o) for o in outs],
            scratch_shapes=[pltpu.VMEM((tok, qc), f32), pltpu.VMEM((tok, 2 * kc), f32)],
        ),
        out_shape=outs,
        cost_estimate=cost(4 * tok * feat * (qc + 2 * kc), 4 * feat * (qc + 2 * kc)),
        name="project_rows",
    )(order, *xs, *sums, qw, kw, vw)


def project_grad(order, gs, total, ow):
    tok, feat = gs[0].shape
    qc = ow.shape[0]

    def body(order_ref, ga, gb, g_in, owr, g_out, acc):
        step = pl.program_id(0)

        def add(g, source, target):
            target[...] = (source[...] + contract(g[...], owr[...], 1, 1)).astype(target.dtype)

        pl.when(step == 0)(lambda: add(ga, g_in, acc))
        pl.when(step == 1)(lambda: add(gb, acc, g_out))

    out = jax.ShapeDtypeStruct((tok, qc), bf16)
    return pl.pallas_call(
        body,
        grid_spec=pltpu.PrefetchScalarGridSpec(
            num_scalar_prefetch=1,
            grid=(2,),
            in_specs=[whole_spec(a) for a in (*gs, total)]
            + [pl.BlockSpec((qc, feat), lambda t, o: (0, o[2 + t]))],
            out_specs=whole_spec(out),
            scratch_shapes=[pltpu.VMEM((tok, qc), f32)],
        ),
        out_shape=out,
        cost_estimate=cost(4 * tok * feat * qc, 4 * feat * qc),
        name="project_grad",
    )(order, *gs, total, ow)


def attention(place, sink, queries, grads, own, low, high):
    tok, qc = queries.shape
    kc = own.shape[1] // 2
    heads = qc // HEAD
    span = tok + 2 * WINDOW

    def body(place_ref, sink_ref, q_ref, g_ref, own_ref, low_ref, high_ref,
             both_out, mine_out, low_out, high_out, sink_out):
        band = jnp.concatenate([low_ref[...], own_ref[...], high_ref[...]], axis=0)
        row = lax.broadcasted_iota(jnp.int32, (tok, span), 0)
        col = lax.broadcasted_iota(jnp.int32, (tok, span), 1)
        start = jnp.where(place_ref[0] == 0, WINDOW, 0)
        stop = jnp.where(place_ref[0] == place_ref[1] - 1, tok + WINDOW, span)
        keep = (col >= row) & (col <= row + 2 * WINDOW) & (col >= start) & (col < stop)
        for kv in range(heads // GROUP):
            at = slice(kv * HEAD, (kv + 1) * HEAD)
            k, v = band[:, at], band[:, kc + kv * HEAD : kc + (kv + 1) * HEAD]
            key_sum = value_sum = None
            for h in range(kv * GROUP, (kv + 1) * GROUP):
                cols = slice(h * HEAD, (h + 1) * HEAD)
                q, g = q_ref[:, cols], g_ref[:, cols]
                scores = jnp.where(keep, contract(q, k, 1, 1) * SCALING, MASKED)
                logit = sink_ref[h]
                top = jnp.maximum(jnp.max(scores, axis=-1, keepdims=True), logit)
                raised = jnp.exp(scores - top)
                sink_raised = jnp.exp(logit - top)
                inverse = 1.0 / (jnp.sum(raised, axis=-1, keepdims=True) + sink_raised)
                soft = raised * inverse
                rounded = soft.astype(bf16)
                attended = contract(rounded, v, 1, 0).astype(bf16)
                dots = jnp.sum(
                    g.astype(f32) * attended.astype(f32), axis=-1, keepdims=True
                )
                score_grads = (soft * (contract(g, v, 1, 1) - dots)).astype(bf16)
                both_out[:, cols] = attended
                both_out[:, qc + h * HEAD : qc + (h + 1) * HEAD] = (
                    contract(score_grads, k, 1, 0) * SCALING
                ).astype(bf16)
                key_part = contract(score_grads, q, 0, 0)
                value_part = contract(rounded, g, 0, 0)
                key_sum = key_part if key_sum is None else key_sum + key_part
                value_sum = value_part if value_sum is None else value_sum + value_part
                part = -jnp.sum(sink_raised * inverse * dots, axis=0, keepdims=True)
                sink_out[h : h + 1, :] = jnp.broadcast_to(part, (1, HEAD))
            for base, total in ((0, key_sum * SCALING), (kc, value_sum)):
                cols = slice(base + kv * HEAD, base + (kv + 1) * HEAD)
                low_out[:, cols] = total[:WINDOW].astype(bf16)
                mine_out[:, cols] = total[WINDOW : WINDOW + tok]
                high_out[:, cols] = total[WINDOW + tok :].astype(bf16)

    outs = [
        jax.ShapeDtypeStruct((tok, 2 * qc), bf16),
        jax.ShapeDtypeStruct((tok, 2 * kc), f32),
        jax.ShapeDtypeStruct((WINDOW, 2 * kc), bf16),
        jax.ShapeDtypeStruct((WINDOW, 2 * kc), bf16),
        jax.ShapeDtypeStruct((heads, HEAD), f32),
    ]
    smem = pl.BlockSpec(memory_space=pltpu.SMEM)
    return pl.pallas_call(
        body,
        in_specs=[smem, smem] + [pl.BlockSpec(memory_space=pltpu.VMEM)] * 5,
        out_specs=[pl.BlockSpec(memory_space=pltpu.VMEM)] * 5,
        out_shape=outs,
        cost_estimate=cost(10 * tok * span * qc * 4, 8 * tok * qc),
        name="attention",
    )(place, sink, queries, grads, own, low, high)


def add_edges(mine, from_next, from_previous):
    tok = mine.shape[0]

    def body(mine_ref, next_ref, previous_ref, out_ref, acc):
        acc[...] = mine_ref[...]
        acc[tok - WINDOW :, :] += next_ref[...].astype(f32)
        acc[:WINDOW, :] += previous_ref[...].astype(f32)
        out_ref[...] = acc[...].astype(bf16)

    return pl.pallas_call(
        body,
        out_shape=jax.ShapeDtypeStruct(mine.shape, bf16),
        scratch_shapes=[pltpu.VMEM(mine.shape, f32)],
        name="add_edges",
    )(mine, from_next, from_previous)


def input_parts(order, both, kv_grads, weights):
    qw, kw, vw = weights
    tok = both.shape[0]
    qc, kc = qw.shape[1], kw.shape[1]
    feat = qw.shape[0] // order.shape[0]

    def body(order_ref, both_ref, kv_ref, *refs):
        for i in range(2):
            qr, kr, vr, out = (*refs[3 * i : 3 * i + 3], refs[6 + i])
            out[0] = (
                contract(both_ref[:, qc:], qr[...], 1, 1)
                + contract(kv_ref[:, :kc], kr[...], 1, 1)
                + contract(kv_ref[:, kc:], vr[...], 1, 1)
            ).astype(bf16)

    rows = lambda cols, side: pl.BlockSpec((feat, cols), lambda t, o: (o[2 * t + side], 0))
    out = jax.ShapeDtypeStruct((2, tok, feat), bf16)
    return pl.pallas_call(
        body,
        grid_spec=pltpu.PrefetchScalarGridSpec(
            num_scalar_prefetch=1,
            grid=(2,),
            in_specs=[whole_spec(both), whole_spec(kv_grads)]
            + [rows(c, side) for side in (0, 1) for c in (qc, kc, kc)],
            out_specs=[pl.BlockSpec((1, tok, feat), lambda t, o: (t, 0, 0))] * 2,
        ),
        out_shape=[out, out],
        cost_estimate=cost(8 * tok * feat * (qc + 2 * kc), 8 * feat * (qc + 2 * kc)),
        name="input_parts",
    )(order, both, kv_grads, *weights, *weights)


def weight_grads(slots, halves, both_blocks, kv_blocks, qc, kc):
    count = len(both_blocks) - 1
    per, arrays, half, width = halves[0].shape
    tok = 2 * half
    tokens = count * tok

    def body(slot_ref, *refs):
        sides = refs[: len(halves)]
        boths = refs[len(halves) : len(halves) + count + 1]
        kvs = refs[len(halves) + count + 1 : len(halves) + 2 * count + 2]
        q_out, k_out, v_out, o_out, x_all, g_all, both_all, kv_all, sem = refs[
            len(halves) + 2 * count + 2 :
        ]
        copies = []

        def start(source, target):
            copies.append(pltpu.make_async_copy(source, target, sem.at[len(copies)]))
            copies[-1].start()

        for n, side in enumerate(sides):
            for i in range(per):
                slot = slot_ref[count + n * per + i]
                start(side.at[i, 0], x_all.at[slot])
                start(side.at[i, 1], g_all.at[slot])
        for blocks, target in ((boths, both_all), (kvs, kv_all)):
            cols = target.shape[2]
            for n, block in enumerate(blocks):
                slot = slot_ref[min(n, count - 1)]
                into = target.at[slot]
                if n == count - 1:
                    into = into.at[:, : cols // 2]
                if n == count:
                    into = into.at[:, cols // 2 :]
                start(block, into)
        for copy in copies:
            copy.wait()
        x = x_all[...].reshape(tokens, width)
        g = g_all[...].reshape(tokens, width)
        o_out[...] = contract(both_all[:, :, :qc].reshape(tokens, qc), g, 0, 0)
        q_out[...] = contract(x, both_all[:, :, qc:].reshape(tokens, qc), 0, 0)
        k_out[...] = contract(x, kv_all[:, :, :kc].reshape(tokens, kc), 0, 0)
        v_out[...] = contract(x, kv_all[:, :, kc:].reshape(tokens, kc), 0, 0)

    hbm = pl.BlockSpec(memory_space=pl.ANY)
    inputs = [*halves, *both_blocks, *kv_blocks]
    n_copies = 2 * per * len(halves) + 2 * (count + 1)
    return pl.pallas_call(
        body,
        in_specs=[pl.BlockSpec(memory_space=pltpu.SMEM)] + [hbm] * len(inputs),
        out_specs=[pl.BlockSpec(memory_space=pltpu.VMEM)] * 4,
        out_shape=[
            jax.ShapeDtypeStruct((width, qc), f32),
            jax.ShapeDtypeStruct((width, kc), f32),
            jax.ShapeDtypeStruct((width, kc), f32),
            jax.ShapeDtypeStruct((qc, width), f32),
        ],
        scratch_shapes=[
            pltpu.VMEM((2 * count, half, width), bf16),
            pltpu.VMEM((2 * count, half, width), bf16),
            pltpu.VMEM((count, tok, 2 * qc), bf16),
            pltpu.VMEM((count, tok, 2 * kc), bf16),
            pltpu.SemaphoreType.DMA((n_copies,)),
        ],
        cost_estimate=cost(2 * tokens * width * (2 * qc + 2 * kc), 8 * tokens * width),
        name="weight_grads",
    )(slots, *inputs)


def slices_of_inputs(own, across):
    count = lax.axis_size("sp")
    r = count // 4
    tok, feat = own[0].shape
    half, width = tok // 2, feat // r
    sp, tp = lax.axis_index("sp"), lax.axis_index("tp")
    high, j_high = sp // (2 * r), tp // 2
    mine = lax.dynamic_slice_in_dim(jnp.stack(own), j_high * half, half, axis=1)
    other = lax.dynamic_slice_in_dim(jnp.stack(across), j_high * half, half, axis=1)
    same = high == j_high
    received = []
    for flip in range(2):
        pairs = []
        for a in range(4):
            for b in range(r):
                for j in range(4):
                    target = (((a // 2) ^ flip) * 2 + j % 2) * r + b
                    pairs.append(((a * r + b) * 4 + j, target * 4 + (j // 2) * 2 + a % 2))
        value = jnp.where(same ^ bool(flip), mine, other)
        received.append(lax.ppermute(value, ("sp", "tp"), pairs))
    stacked = jnp.stack(received)
    b = sp % r
    parts = []
    for step in range(r):
        to = b ^ step
        value = lax.dynamic_slice_in_dim(stacked, to * width, width, axis=3)
        if step:
            pairs = [(i, i - i % r + ((i % r) ^ step)) for i in range(count)]
            value = lax.ppermute(value, "sp", pairs)
        parts.append(value)
    near = jnp.concatenate(parts)
    far = swap_tp(near, 2)
    return [near, far, swap_tp(near, 1), swap_tp(far, 1)]


def block_slots():
    count = lax.axis_size("sp")
    r = count // 4
    order = ring_order(count)
    position = [order.index(i) for i in range(count)]
    sp, tp = lax.axis_index("sp"), lax.axis_index("tp")
    offsets = [0]
    for s in range(1, count // 2):
        offsets += [-s, s]
    offsets.append(count // 2)
    here = jnp.asarray(position, jnp.int32)[sp]
    ring = jnp.asarray(order, jnp.int32)[(here + jnp.asarray(offsets, jnp.int32)) % count]
    n = jnp.arange(8 * r, dtype=jnp.int32)
    flip, step, far, core = n % 2, n // 2 % r, n // (2 * r) % 2, n // (4 * r)
    token_block = (
        ((sp // (2 * r)) ^ flip) * 2 * r + ((tp % 2) ^ core) * r + ((sp % r) ^ step)
    )
    return jnp.concatenate([ring, token_block * 2 + ((tp // 2) ^ far)])


def sum_over_sp(value):
    count = lax.axis_size("sp")
    if count & (count - 1):
        return lax.psum(value, "sp")
    bit = 1
    while bit < count:
        value = value + lax.ppermute(value, "sp", [(i, i ^ bit) for i in range(count)])
        bit *= 2
    return value


def per_device(
    layer_input, output_grad, query_weight, key_weight, value_weight, out_weight, sink_logit
):
    count = lax.axis_size("sp")
    qc, kc = query_weight.shape[1], key_weight.shape[1]
    tok = layer_input.shape[0]
    depth = query_weight.shape[0]
    tp, sp = lax.axis_index("tp"), lax.axis_index("sp")
    order = tp ^ jnp.arange(4, dtype=jnp.int32)
    place = jnp.stack([sp, jnp.int32(count)])
    rows_weights = (query_weight, key_weight, value_weight)

    x_y, g_y = swap_tp(layer_input, 2), swap_tp(output_grad, 2)
    x_c, g_c = swap_tp(layer_input, 1), swap_tp(output_grad, 1)
    x_yc, g_yc = swap_tp(x_y, 1), swap_tp(g_y, 1)
    q_sum, kv_sum, g_sum = project_first(
        order, (layer_input, x_c), (output_grad, g_c), (*rows_weights, out_weight)
    )
    queries, key_values = project_rows(order, (x_y, x_yc), (q_sum, kv_sum), rows_weights)
    low = passed_along(key_values[tok - WINDOW :], 1)
    high = passed_along(key_values[:WINDOW], -1)
    grads = project_grad(order, (g_y, g_yc), g_sum, out_weight)

    both, mine, to_previous, to_next, sink_part = attention(
        place, sink_logit, queries, grads, key_values, low, high
    )
    from_next = passed_along(to_previous, -1)
    from_previous = passed_along(to_next, 1)
    kv_grads = add_edges(mine, from_next, from_previous)
    sink_grad = sum_over_sp(sink_part)[:, 0]

    kept, sent = input_parts(order, both, kv_grads, rows_weights)
    kept = (kept.astype(f32) + swap_tp(sent, 1).astype(f32)).astype(bf16)
    input_grad = (kept[0].astype(f32) + swap_tp(kept[1], 2).astype(f32)).astype(bf16)

    gathered = count * tok * (2 * depth // count + 2 * qc + 2 * kc) * 2
    if gathered < depth * (2 * qc + 2 * kc) * 4 and (depth // count) % 128 == 0:
        halves = slices_of_inputs((layer_input, output_grad), (x_y, g_y))
        q_part, k_part, v_part, o_part = weight_grads(
            block_slots(), halves, ring_gather(both), ring_gather(kv_grads), qc, kc
        )
    else:
        blocks = lambda *parts: jnp.concatenate(
            [lax.dynamic_index_in_dim(jnp.stack(parts), tp ^ i, keepdims=False)
             for i in range(4)], axis=1)
        whole_input = blocks(layer_input, x_c, x_y, x_yc)
        whole_grad = blocks(output_grad, g_c, g_y, g_yc)
        sums = jnp.concatenate(
            [
                contract(whole_input, both[:, qc:], 0, 0),
                contract(whole_grad, both[:, :qc], 0, 0),
                contract(whole_input, kv_grads, 0, 0),
            ],
            axis=1,
        )
        sums = lax.psum_scatter(sums, "sp", scatter_dimension=0, tiled=True)
        q_part, o_part = sums[:, :qc], sums[:, qc : 2 * qc].T
        k_part = sums[:, 2 * qc : 2 * qc + kc]
        v_part = sums[:, 2 * qc + kc :]
    return (input_grad, q_part, k_part, v_part, o_part, sink_grad)


def solution(mesh):
    placed = (
        P("sp", "tp"),
        P("sp", "tp"),
        P(None, "tp"),
        P(None, "tp"),
        P(None, "tp"),
        P("tp", None),
        P("tp"),
    )
    return jax.shard_map(
        per_device,
        mesh=mesh,
        in_specs=placed,
        out_specs=(
            P("sp", "tp"),
            P("sp", "tp"),
            P("sp", "tp"),
            P("sp", "tp"),
            P("tp", "sp"),
            P("tp"),
        ),
        check_vma=False,
    )
```

```python
import jax
import jax.numpy as jnp
from jax import lax
from jax.experimental import pallas as pl
from jax.experimental.pallas import tpu as pltpu
from jax.sharding import PartitionSpec as P


HEADS = 16
KV_HEADS = 8
HEAD = 128
WINDOW = 128
GROUP = HEADS // KV_HEADS
SCALING = HEAD ** (-0.5)
MASKED = -1e30


bf16 = jnp.bfloat16
f32 = jnp.float32


def contract(left, right, ldim, rdim):
    return lax.dot_general(
        left, right, (((ldim,), (rdim,)), ((), ())), preferred_element_type=f32
    )


def on_chip(*arrays):
    return [pltpu.with_memory_space_constraint(a, pltpu.VMEM) for a in arrays]


VMEM = pl.BlockSpec(memory_space=pltpu.VMEM)
SMEM = pl.BlockSpec(memory_space=pltpu.SMEM)
HBM = pl.BlockSpec(memory_space=pltpu.HBM)


def off_chip(*arrays):
    return [pltpu.with_memory_space_constraint(a, pltpu.HBM) for a in arrays]


def grant(mib):
    return pltpu.CompilerParams(vmem_limit_bytes=mib * 2**20)


def cost(flops, moved):
    return pl.CostEstimate(flops=flops, transcendentals=0, bytes_accessed=moved)


def swap_tp(value, bit):
    return lax.ppermute(value, "tp", [(i, i ^ bit) for i in range(lax.axis_size("tp"))])


def ring_order(count):
    return list(range(0, count, 2)) + list(range(1, count, 2))[::-1]


def ring_shift(value, steps):
    count = lax.axis_size("sp")
    order = ring_order(count)
    pairs = [(order[p], order[(p + steps) % count]) for p in range(count)]
    return lax.ppermute(value, "sp", pairs)


def swap_sp(value, odd):
    count = lax.axis_size("sp")
    pairs = []
    for i in range(odd, count - 1, 2):
        pairs += [(i, i + 1), (i + 1, i)]
    return lax.ppermute(value, "sp", pairs)


def ring_gather(value):
    count = lax.axis_size("sp")
    blocks, forward, backward = [value], value, value
    for _ in range(1, count // 2):
        forward = ring_shift(forward, 1)
        backward = ring_shift(backward, -1)
        blocks += [forward, backward]
    half = value.shape[1] // 2
    forward, backward = forward[:, :half], backward[:, half:]
    blocks += [ring_shift(forward, 1),
               ring_shift(backward, -1)]
    return blocks


SINK_ROWS = 8


def stage(layer_input, output_grad, *weights):
    arrays = (layer_input, output_grad, *weights)
    count = len(arrays)

    def body(*refs):
        sources, targets, sem = refs[:count], refs[count : 2 * count], refs[-1]
        copies = [
            pltpu.make_async_copy(a, b, sem.at[n]) for n, (a, b) in enumerate(zip(sources, targets))
        ]
        for copy in copies:
            copy.start()
        for copy in copies:
            copy.wait()

    return pl.pallas_call(
        body,
        in_specs=[HBM] * count,
        out_specs=[VMEM] * count,
        out_shape=[pltpu.VMEM(a.shape, a.dtype) for a in arrays],
        scratch_shapes=[pltpu.SemaphoreType.DMA((count,))],
        cost_estimate=cost(10**9, 12 * 2**20),
        compiler_params=grant(2),
        name="stage",
    )(*off_chip(*arrays))


def rows_part(place, xs, start, sums, weights, final):
    tok, feat = xs[0].shape
    qw, kw, vw = weights
    qc, kc = qw.shape[1], kw.shape[1]

    def body(place_ref, *refs):
        x_refs, sum_refs, refs = refs[:2], refs[2 : 2 + len(sums)], refs[2 + len(sums) :]
        qr, kr, vr, q_out, kv_out = refs[:5]
        targets = (
            (0, q_out, slice(None), qr),
            (1, kv_out, slice(0, kc), kr),
            (1, kv_out, slice(kc, 2 * kc), vr),
        )
        for which, out, cols, w in targets:
            value = sum_refs[which][:, cols] if sums else None
            for n, x in enumerate(x_refs):
                at = pl.multiple_of((place_ref[1] ^ (start + n)) * feat, feat)
                part = contract(x[...], w[pl.ds(at, feat), :], 1, 0)
                value = part if value is None else value + part
            out[:, cols] = value.astype(out.dtype)
        if final:
            first, second = refs[5:]
            even = place_ref[0] % 2 == 0

            @pl.when(even)
            def _():
                first[...] = kv_out[tok - WINDOW :, :]
                second[...] = kv_out[:WINDOW, :]

            @pl.when(jnp.logical_not(even))
            def _():
                first[...] = kv_out[:WINDOW, :]
                second[...] = kv_out[tok - WINDOW :, :]

    edges = [pltpu.VMEM((WINDOW, 2 * kc), bf16)] * (2 * final)
    dtype = bf16 if final else f32
    return pl.pallas_call(
        body,
        in_specs=[SMEM] + [VMEM] * (5 + len(sums)),
        out_specs=[VMEM] * (2 + len(edges)),
        out_shape=[pltpu.VMEM((tok, qc), dtype), pltpu.VMEM((tok, 2 * kc), dtype), *edges],
        cost_estimate=cost(4 * tok * feat * (qc + 2 * kc), 4 * feat * (qc + 2 * kc)),
        compiler_params=grant(8),
        name="rows_part",
    )(place, *on_chip(*xs, *sums, qw, kw, vw))


def grad_part(place, gs, start, sums, ow, final):
    tok, feat = gs[0].shape
    qc = ow.shape[0]

    def body(place_ref, *refs):
        g_refs, sum_refs, (owr, out) = refs[:2], refs[2 : 2 + len(sums)], refs[2 + len(sums) :]
        value = sum_refs[0][...] if sums else None
        for n, g in enumerate(g_refs):
            at = pl.multiple_of((place_ref[1] ^ (start + n)) * feat, feat)
            part = contract(owr[:, pl.ds(at, feat)], g[...], 1, 1)
            value = part if value is None else value + part
        out[...] = value.T.astype(out.dtype) if final else value

    return pl.pallas_call(
        body,
        in_specs=[SMEM] + [VMEM] * (3 + len(sums)),
        out_specs=VMEM,
        out_shape=pltpu.VMEM((tok, qc), bf16) if final else pltpu.VMEM((qc, tok), f32),
        cost_estimate=cost(4 * tok * feat * qc, 4 * feat * qc),
        compiler_params=grant(6),
        name="grad_part",
    )(place, *on_chip(*gs, *sums, ow))


def attention(place, sink, queries, grads, own, first, second):
    tok, qc = queries.shape
    kc = own.shape[1] // 2
    heads = qc // HEAD
    span = tok + 2 * WINDOW
    count = lax.axis_size("sp")

    def body(place_ref, sink_ref, q_ref, g_ref, own_ref, first_ref, second_ref,
             both_out, mine_out, first_out, second_out, sink_out):
        even = place_ref[0] % 2 == 0
        low = jnp.where(even, second_ref[...], first_ref[...])
        high = jnp.where(even, first_ref[...], second_ref[...])
        band = jnp.concatenate([low, own_ref[...], high], axis=0)
        row = lax.broadcasted_iota(jnp.int32, (tok, span), 0)
        col = lax.broadcasted_iota(jnp.int32, (tok, span), 1)
        start = jnp.where(place_ref[0] == 0, WINDOW, 0)
        stop = jnp.where(place_ref[0] == count - 1, tok + WINDOW, span)
        keep = (col >= row) & (col <= row + 2 * WINDOW) & (col >= start) & (col < stop)
        for kv in range(heads // GROUP):
            at = slice(kv * HEAD, (kv + 1) * HEAD)
            k, v = band[:, at], band[:, kc + kv * HEAD : kc + (kv + 1) * HEAD]
            key_sum = value_sum = None
            for h in range(kv * GROUP, (kv + 1) * GROUP):
                cols = slice(h * HEAD, (h + 1) * HEAD)
                q, g = q_ref[:, cols], g_ref[:, cols]
                scores = jnp.where(keep, contract(q, k, 1, 1) * SCALING, MASKED)
                logit = sink_ref[h]
                top = jnp.maximum(jnp.max(scores, axis=-1, keepdims=True), logit)
                raised = jnp.exp(scores - top)
                sink_raised = jnp.exp(logit - top)
                inverse = 1.0 / (jnp.sum(raised, axis=-1, keepdims=True) + sink_raised)
                soft = raised * inverse
                rounded = soft.astype(bf16)
                attended = contract(rounded, v, 1, 0).astype(bf16)
                dots = jnp.sum(
                    g.astype(f32) * attended.astype(f32), axis=-1, keepdims=True
                )
                score_grads = (soft * (contract(g, v, 1, 1) - dots)).astype(bf16)
                both_out[:, cols] = attended
                both_out[:, qc + h * HEAD : qc + (h + 1) * HEAD] = (
                    contract(score_grads, k, 1, 0) * SCALING
                ).astype(bf16)
                key_part = contract(score_grads, q, 0, 0)
                value_part = contract(rounded, g, 0, 0)
                key_sum = key_part if key_sum is None else key_sum + key_part
                value_sum = value_part if value_sum is None else value_sum + value_part
                part = -jnp.sum(sink_raised * inverse * dots, axis=0, keepdims=True)
                sink_out[:, cols] = jnp.broadcast_to(part, (SINK_ROWS, HEAD))
            for base, total in ((0, key_sum * SCALING), (kc, value_sum)):
                cols = slice(base + kv * HEAD, base + (kv + 1) * HEAD)
                low = total[:WINDOW].astype(bf16)
                high = total[WINDOW + tok :].astype(bf16)
                first_out[:, cols] = jnp.where(even, high, low)
                second_out[:, cols] = jnp.where(even, low, high)
                mine_out[:, cols] = total[WINDOW : WINDOW + tok]

    outs = [
        pltpu.VMEM((tok, 2 * qc), bf16),
        pltpu.VMEM((tok, 2 * kc), f32),
        pltpu.VMEM((WINDOW, 2 * kc), bf16),
        pltpu.VMEM((WINDOW, 2 * kc), bf16),
        pltpu.VMEM((SINK_ROWS, qc), f32),
    ]
    return pl.pallas_call(
        body,
        in_specs=[SMEM, SMEM] + [VMEM] * 5,
        out_specs=[VMEM] * 5,
        out_shape=outs,
        cost_estimate=cost(10 * tok * span * qc * 4, 8 * tok * qc),
        name="attention",
        compiler_params=grant(16),
    )(place, sink, *on_chip(queries, grads, own, first, second))


def add_edges(place, mine, first, second, sink_part):
    tok, cols = mine.shape

    def body(place_ref, mine_ref, first_ref, second_ref, sink_ref, out_ref, acc):
        even = place_ref[0] % 2 == 0
        one, other = first_ref[...].astype(f32), second_ref[...].astype(f32)
        acc[...] = mine_ref[...]
        acc[tok - WINDOW :, :] += jnp.where(even, one, other)
        acc[:WINDOW, :] += jnp.where(even, other, one)
        out_ref[:tok, :] = acc[...].astype(bf16)
        row = lax.broadcasted_iota(jnp.int32, (SINK_ROWS, cols), 0)
        left = sink_ref[...]
        pieces = jnp.zeros((SINK_ROWS, cols), f32)
        for n in range(3):
            piece = left.astype(bf16).astype(f32)
            pieces = jnp.where(row == n, piece, pieces)
            left = left - piece
        out_ref[tok:, :] = pieces.astype(bf16)

    return pl.pallas_call(
        body,
        in_specs=[SMEM] + [VMEM] * 4,
        out_specs=VMEM,
        out_shape=pltpu.VMEM((tok + SINK_ROWS, cols), bf16),
        scratch_shapes=[pltpu.VMEM(mine.shape, f32)],
        cost_estimate=cost(tok * cols * 100, 8 * tok * cols),
        name="add_edges",
        compiler_params=grant(4),
    )(place, *on_chip(mine, first, second, sink_part))


def input_parts(place, both, kv_grads, weights):
    qw, kw, _ = weights
    tok = both.shape[0]
    qc, kc = qw.shape[1], kw.shape[1]
    feat = qw.shape[0] // 4

    def body(place_ref, both_ref, kv_ref, qr, kr, vr, sent, kept):
        for out, index, away in ((sent, 0, 1), (sent, 1, 3), (kept, 0, 0), (kept, 1, 2)):
            at = pl.ds(pl.multiple_of((place_ref[1] ^ away) * feat, feat), feat)
            out[index] = (
                contract(qr[at, :], both_ref[:, qc:], 1, 1)
                + contract(kr[at, :], kv_ref[:tok, :kc], 1, 1)
                + contract(vr[at, :], kv_ref[:tok, kc:], 1, 1)
            ).T.astype(bf16)

    out = pltpu.VMEM((2, tok, feat), bf16)
    return pl.pallas_call(
        body,
        in_specs=[SMEM] + [VMEM] * 5,
        out_specs=[VMEM, VMEM],
        out_shape=[out, out],
        cost_estimate=cost(8 * tok * feat * (qc + 2 * kc), 8 * feat * (qc + 2 * kc)),
        compiler_params=grant(10),
        name="input_parts",
    )(place, *on_chip(both, kv_grads, *weights))


def token_block(place_ref, offset, count):
    own = place_ref[0]
    position = jnp.where(own % 2 == 0, own // 2, count - 1 - own // 2) + offset
    position = jnp.where(position < 0, position + count, position)
    position = jnp.where(position >= count, position - count, position)
    return jnp.where(position < count // 2, 2 * position, 2 * (count - 1 - position) + 1)


def side_index(place_ref, block, half, r):
    own, tp = place_ref[0], place_ref[1]
    core = (block // r % 2) ^ (tp % 2)
    far = half ^ (tp // 2)
    step = (block % r) ^ (own % r)
    flip = (block // (2 * r)) ^ (own // (2 * r))
    return ((core * 2 + far) * r + step) * 2 + flip


def weights_early(place, sides, boths, kvs, qc, kc):
    count = len(boths) + 1
    r = count // 4
    half, width = sides.shape[2:]
    tok = 2 * half

    def body(place_ref, side_ref, *refs):
        both_refs, kv_refs = refs[: count - 1], refs[count - 1 : 2 * count - 2]
        q_out, kv_out, o_out, sink_out, x_all, g_all, both_all, kv_all = refs[2 * count - 2 :]
        for n in range(count - 1):
            offset = (n + 1) // 2 * (-1 if n % 2 else 1)
            block = token_block(place_ref, offset, count)
            for i in range(2):
                at = side_index(place_ref, block, i, r)
                rows = slice(n * tok + i * half, n * tok + (i + 1) * half)
                x_all[rows, :] = side_ref[at, 0]
                g_all[rows, :] = side_ref[at, 1]
            rows = slice(n * tok, (n + 1) * tok)
            both_all[rows, :] = both_refs[n][...]
            kv_all[rows, :] = kv_refs[n][:tok, :]
            sink_out[block] = kv_refs[n][tok:, :]
        o_out[...] = contract(both_all[:, :qc], g_all[...], 0, 0)
        q_out[...] = contract(x_all[...], both_all[:, qc:], 0, 0)
        kv_out[...] = contract(x_all[...], kv_all[...], 0, 0)

    tokens = (count - 1) * tok
    return pl.pallas_call(
        body,
        in_specs=[SMEM] + [VMEM] * (2 * count - 1),
        out_specs=[VMEM] * 4,
        out_shape=[
            pltpu.VMEM((width, qc), f32),
            pltpu.VMEM((width, 2 * kc), f32),
            pltpu.VMEM((qc, width), f32),
            pltpu.VMEM((count, SINK_ROWS, 2 * kc), bf16),
        ],
        scratch_shapes=[
            pltpu.VMEM((tokens, width), bf16),
            pltpu.VMEM((tokens, width), bf16),
            pltpu.VMEM((tokens, 2 * qc), bf16),
            pltpu.VMEM((tokens, 2 * kc), bf16),
        ],
        cost_estimate=cost(2 * tokens * width * (2 * qc + 2 * kc), 8 * tokens * width),
        name="weights_early",
        compiler_params=grant(20),
    )(place, *on_chip(sides, *boths, *kvs))


def weights_late(place, sides, both_halves, kv_halves, sums, sinks, qc, kc):
    count = sinks.shape[0]
    r = count // 4
    half, width = sides.shape[2:]
    tok = 2 * half

    def body(place_ref, side_ref, att, dq, dk, dv, q_in, kv_in, o_in, sink_in,
             q_out, k_out, v_out, o_out, sink_out):
        block = token_block(place_ref, count // 2, count)
        at = [side_index(place_ref, block, i, r) for i in range(2)]
        x = jnp.concatenate([side_ref[i, 0] for i in at], axis=0)
        g = jnp.concatenate([side_ref[i, 1] for i in at], axis=0)
        o_out[...] = o_in[...] + contract(att[...], g, 0, 0)
        q_out[...] = q_in[...] + contract(x, dq[...], 0, 0)
        k_out[...] = kv_in[:, :kc] + contract(x, dk[:tok, :], 0, 0)
        v_out[...] = kv_in[:, kc:] + contract(x, dv[:tok, :], 0, 0)
        last = jnp.concatenate([dk[tok:, :], dv[tok:, :]], axis=1).astype(f32)
        total = None
        for n in range(count):
            rows = jnp.where(block == n, last, sink_in[n].astype(f32))
            value = rows[0:1] + rows[1:2] + rows[2:3]
            total = value if total is None else total + value
        for h in range(qc // HEAD):
            sink_out[h] = jnp.max(total[:, h * HEAD : (h + 1) * HEAD])

    shapes = [(width, qc), (width, kc), (width, kc), (qc, width)]
    return pl.pallas_call(
        body,
        in_specs=[SMEM] + [VMEM] * 9,
        out_specs=[VMEM] * 4 + [SMEM],
        out_shape=[jax.ShapeDtypeStruct(shape, f32) for shape in (*shapes, (qc // HEAD,))],
        cost_estimate=cost(2 * tok * width * (2 * qc + 2 * kc), 16 * width * qc),
        compiler_params=grant(12),
        name="weights_late",
    )(place, *on_chip(sides, *both_halves, *kv_halves, *sums, sinks))


def block_halves(place, own, across):
    tok, feat = own[0].shape
    r = lax.axis_size("sp") // 4
    half, width = tok // 2, feat // r

    def body(place_ref, own_x, own_g, across_x, across_g, *outs):
        high = place_ref[1] // 2
        rows = pl.ds(pl.multiple_of(high * half, half), half)
        same = place_ref[0] // (2 * r) == high

        def cut(sources):
            for n, out in enumerate(outs):
                at = pl.multiple_of(((place_ref[0] % r) ^ (n % r)) * width, width)
                for i, source in enumerate(sources[n // r]):
                    out[i] = source[rows, pl.ds(at, width)]

        here, there = (own_x, own_g), (across_x, across_g)
        pl.when(same)(lambda: cut((here, there)))
        pl.when(jnp.logical_not(same))(lambda: cut((there, here)))

    outs = pl.pallas_call(
        body,
        in_specs=[SMEM] + [VMEM] * 4,
        out_specs=[VMEM] * (2 * r),
        out_shape=[pltpu.VMEM((2, half, width), bf16)] * (2 * r),
        cost_estimate=cost(10**7, 8 * tok * feat),
        compiler_params=grant(2),
        name="block_halves",
    )(place, *on_chip(*own, *across))
    return outs[:r], outs[r:]


def send_half(flip, step, value):
    count = lax.axis_size("sp")
    r = count // 4
    pairs = []
    for a in range(4):
        for b in range(r):
            for j in range(4):
                target = (((a // 2) ^ flip) * 2 + j % 2) * r + (b ^ step)
                pairs.append(((a * r + b) * 4 + j, target * 4 + (j // 2) * 2 + a % 2))
    return lax.ppermute(value, ("sp", "tp"), pairs)


def stack_near(pieces):
    def body(*refs):
        for n, ref in enumerate(refs[:-1]):
            refs[-1][n] = ref[...]

    return pl.pallas_call(
        body,
        in_specs=[VMEM] * len(pieces),
        out_specs=VMEM,
        out_shape=pltpu.VMEM((len(pieces), *pieces[0].shape), bf16),
        cost_estimate=cost(10**7, 2**21),
        compiler_params=grant(2),
        name="stack_near",
    )(*on_chip(*pieces))


def spread_slices(near):
    near = stack_near(near)
    far = swap_tp(near, 2)
    sides = jnp.stack([near, far, swap_tp(near, 1), swap_tp(far, 1)])
    return sides.reshape(-1, *near.shape[1:])


def gathers_operands(count, tok, depth, qc, kc):
    gathered = count * tok * (2 * depth // count + 2 * qc + 2 * kc) * 2
    return (
        gathered < depth * (2 * qc + 2 * kc) * 4
        and (depth // count) % 128 == 0
        and count % 4 == 0
        and qc == 2 * kc
    )


def layer_backward(
    layer_input, output_grad, query_weight, key_weight, value_weight, out_weight, sink_logit
):
    count = lax.axis_size("sp")
    qc, kc = query_weight.shape[1], key_weight.shape[1]
    tok = layer_input.shape[0]
    depth = query_weight.shape[0]
    tp, sp = lax.axis_index("tp"), lax.axis_index("sp")
    place = jnp.stack([sp, tp])
    gathers = gathers_operands(count, tok, depth, qc, kc)

    x_y, g_y = swap_tp(layer_input, 2), swap_tp(output_grad, 2)
    x_c, g_c = swap_tp(layer_input, 1), swap_tp(output_grad, 1)
    own_x, own_g, *rows_weights, out_weight = stage(
        layer_input, output_grad, query_weight, key_weight, value_weight, out_weight
    )
    if gathers:
        stay, leave = block_halves(place, (own_x, own_g), (x_y, g_y))
        near = []
        for step in range(count // 4):
            near += [send_half(0, step, stay[step]), send_half(1, step, leave[step])]
    x_yc, g_yc = swap_tp(x_y, 1), swap_tp(g_y, 1)
    row_sums = rows_part(place, (own_x, x_c), 0, (), rows_weights, False)
    queries, key_values, first, second = rows_part(place, (x_y, x_yc), 2, row_sums, rows_weights, True)
    first, second = swap_sp(first, 0), swap_sp(second, 1)
    grad_sum = grad_part(place, (own_g, g_c), 0, (), out_weight, False)
    grads = grad_part(place, (g_y, g_yc), 2, (grad_sum,), out_weight, True)

    both, mine, first, second, sink_part = attention(
        place, sink_logit, queries, grads, key_values, first, second
    )
    first, second = swap_sp(first, 0), swap_sp(second, 1)
    kv_grads = add_edges(place, mine, first, second, sink_part)

    sent, kept = input_parts(place, both, kv_grads, rows_weights)
    kept = (kept.astype(f32) + swap_tp(sent, 1).astype(f32)).astype(bf16)
    from_far = swap_tp(kept[1], 2)
    input_grad = (kept[0].astype(f32) + from_far.astype(f32)).astype(bf16)

    if gathers:
        sides = spread_slices(near)
        boths, kvs = ring_gather(both), ring_gather(kv_grads)
        *sums, sinks = weights_early(place, sides, boths[:-2], kvs[:-2], qc, kc)
        q_part, k_part, v_part, o_part, sink_grad = weights_late(
            place, sides, boths[-2:], kvs[-2:], sums, sinks, qc, kc
        )
    else:
        blocks = lambda *parts: jnp.concatenate(
            [lax.dynamic_index_in_dim(jnp.stack(parts), tp ^ i, keepdims=False)
             for i in range(4)], axis=1)
        whole_input = blocks(layer_input, x_c, x_y, x_yc)
        whole_grad = blocks(output_grad, g_c, g_y, g_yc)
        sums = jnp.concatenate(
            [
                contract(whole_input, both[:, qc:], 0, 0),
                contract(whole_grad, both[:, :qc], 0, 0),
                contract(whole_input, kv_grads[:tok], 0, 0),
            ],
            axis=1,
        )
        sums = lax.psum_scatter(sums, "sp", scatter_dimension=0, tiled=True)
        q_part, o_part = sums[:, :qc], sums[:, qc : 2 * qc].T
        k_part = sums[:, 2 * qc : 2 * qc + kc]
        v_part = sums[:, 2 * qc + kc :]
        sink_grad = lax.psum(sink_part[0, ::HEAD], "sp")
    return (input_grad, q_part, k_part, v_part, o_part, sink_grad)


def solution(mesh):
    placed = (
        P("sp", "tp"),
        P("sp", "tp"),
        P(None, "tp"),
        P(None, "tp"),
        P(None, "tp"),
        P("tp", None),
        P("tp"),
    )
    return jax.shard_map(
        layer_backward,
        mesh=mesh,
        in_specs=placed,
        out_specs=(
            P("sp", "tp"),
            P("sp", "tp"),
            P("sp", "tp"),
            P("sp", "tp"),
            P("tp", "sp"),
            P("tp"),
        ),
        check_vma=False,
    )
```

```python
import jax
import jax.numpy as jnp
from jax import lax
from jax.experimental import pallas as pl
from jax.experimental.pallas import tpu as pltpu
from jax.sharding import PartitionSpec as P


HEADS = 16
KV_HEADS = 8
HEAD = 128
WINDOW = 128
GROUP = HEADS // KV_HEADS
SCALING = HEAD ** (-0.5)
MASKED = -1e30


bf16 = jnp.bfloat16
f32 = jnp.float32


def contract(left, right, ldim, rdim):
    return lax.dot_general(
        left, right, (((ldim,), (rdim,)), ((), ())), preferred_element_type=f32
    )


def on_chip(*arrays):
    return [pltpu.with_memory_space_constraint(a, pltpu.VMEM) for a in arrays]


VMEM = pl.BlockSpec(memory_space=pltpu.VMEM)
SMEM = pl.BlockSpec(memory_space=pltpu.SMEM)
HBM = pl.BlockSpec(memory_space=pltpu.HBM)


def off_chip(*arrays):
    return [pltpu.with_memory_space_constraint(a, pltpu.HBM) for a in arrays]


def grant(mib):
    return pltpu.CompilerParams(vmem_limit_bytes=mib * 2**20)


def cost(flops, moved):
    return pl.CostEstimate(flops=flops, transcendentals=0, bytes_accessed=moved)


def swap_tp(value, bit):
    return lax.ppermute(value, "tp", [(i, i ^ bit) for i in range(lax.axis_size("tp"))])


def ring_order(count):
    return list(range(0, count, 2)) + list(range(1, count, 2))[::-1]


def ring_shift(value, steps):
    count = lax.axis_size("sp")
    order = ring_order(count)
    pairs = [(order[p], order[(p + steps) % count]) for p in range(count)]
    return lax.ppermute(value, "sp", pairs)


def swap_sp(value, odd):
    count = lax.axis_size("sp")
    pairs = []
    for i in range(odd, count - 1, 2):
        pairs += [(i, i + 1), (i + 1, i)]
    return lax.ppermute(value, "sp", pairs)


def ring_gather(value):
    count = lax.axis_size("sp")
    blocks, forward, backward = [value], value, value
    for _ in range(1, count // 2):
        forward = ring_shift(forward, 1)
        backward = ring_shift(backward, -1)
        blocks += [forward, backward]
    half = value.shape[1] // 2
    forward, backward = forward[:, :half], backward[:, half:]
    blocks += [ring_shift(forward, 1),
               ring_shift(backward, -1)]
    return blocks


SINK_ROWS = 8


def stage(layer_input, output_grad, *weights):
    arrays = (layer_input, output_grad, *weights)
    count = len(arrays)

    def body(*refs):
        sources, targets, sem = refs[:count], refs[count : 2 * count], refs[-1]
        copies = [
            pltpu.make_async_copy(a, b, sem.at[n]) for n, (a, b) in enumerate(zip(sources, targets))
        ]
        for copy in copies:
            copy.start()
        for copy in copies:
            copy.wait()

    return pl.pallas_call(
        body,
        in_specs=[HBM] * count,
        out_specs=[VMEM] * count,
        out_shape=[pltpu.VMEM(a.shape, a.dtype) for a in arrays],
        scratch_shapes=[pltpu.SemaphoreType.DMA((count,))],
        cost_estimate=cost(10**9, 12 * 2**20),
        compiler_params=grant(2),
        name="stage",
    )(*off_chip(*arrays))


def rows_part(place, xs, start, sums, weights, final):
    tok, feat = xs[0].shape
    qw, kw, vw = weights
    qc, kc = qw.shape[1], kw.shape[1]

    def body(place_ref, *refs):
        x_refs, sum_refs, refs = refs[:2], refs[2 : 2 + len(sums)], refs[2 + len(sums) :]
        qr, kr, vr, q_out, kv_out = refs[:5]
        targets = (
            (0, q_out, slice(None), qr),
            (1, kv_out, slice(0, kc), kr),
            (1, kv_out, slice(kc, 2 * kc), vr),
        )
        for which, out, cols, w in targets:
            value = sum_refs[which][:, cols] if sums else None
            for n, x in enumerate(x_refs):
                at = pl.multiple_of((place_ref[1] ^ (start + n)) * feat, feat)
                part = contract(x[...], w[pl.ds(at, feat), :], 1, 0)
                value = part if value is None else value + part
            out[:, cols] = value.astype(out.dtype)
        if final:
            first, second = refs[5:]
            even = place_ref[0] % 2 == 0

            @pl.when(even)
            def _():
                first[...] = kv_out[tok - WINDOW :, :]
                second[...] = kv_out[:WINDOW, :]

            @pl.when(jnp.logical_not(even))
            def _():
                first[...] = kv_out[:WINDOW, :]
                second[...] = kv_out[tok - WINDOW :, :]

    edges = [pltpu.VMEM((WINDOW, 2 * kc), bf16)] * (2 * final)
    dtype = bf16 if final else f32
    return pl.pallas_call(
        body,
        in_specs=[SMEM] + [VMEM] * (5 + len(sums)),
        out_specs=[VMEM] * (2 + len(edges)),
        out_shape=[pltpu.VMEM((tok, qc), dtype), pltpu.VMEM((tok, 2 * kc), dtype), *edges],
        cost_estimate=cost(4 * tok * feat * (qc + 2 * kc), 4 * feat * (qc + 2 * kc)),
        compiler_params=grant(8),
        name="rows_part",
    )(place, *on_chip(*xs, *sums, qw, kw, vw))


def grad_part(place, gs, start, sums, ow, final):
    tok, feat = gs[0].shape
    qc = ow.shape[0]

    def body(place_ref, *refs):
        g_refs, sum_refs, (owr, out) = refs[:2], refs[2 : 2 + len(sums)], refs[2 + len(sums) :]
        value = sum_refs[0][...] if sums else None
        for n, g in enumerate(g_refs):
            at = pl.multiple_of((place_ref[1] ^ (start + n)) * feat, feat)
            part = contract(owr[:, pl.ds(at, feat)], g[...], 1, 1)
            value = part if value is None else value + part
        out[...] = value.T.astype(out.dtype) if final else value

    return pl.pallas_call(
        body,
        in_specs=[SMEM] + [VMEM] * (3 + len(sums)),
        out_specs=VMEM,
        out_shape=pltpu.VMEM((tok, qc), bf16) if final else pltpu.VMEM((qc, tok), f32),
        cost_estimate=cost(4 * tok * feat * qc, 4 * feat * qc),
        compiler_params=grant(6),
        name="grad_part",
    )(place, *on_chip(*gs, *sums, ow))


def attention(place, sink, queries, grads, own, first, second):
    tok, qc = queries.shape
    kc = own.shape[1] // 2
    heads = qc // HEAD
    span = tok + 2 * WINDOW
    count = lax.axis_size("sp")

    def body(place_ref, sink_ref, q_ref, g_ref, own_ref, first_ref, second_ref,
             both_out, mine_out, first_out, second_out, sink_out):
        even = place_ref[0] % 2 == 0
        low = jnp.where(even, second_ref[...], first_ref[...])
        high = jnp.where(even, first_ref[...], second_ref[...])
        band = jnp.concatenate([low, own_ref[...], high], axis=0)
        row = lax.broadcasted_iota(jnp.int32, (tok, span), 0)
        col = lax.broadcasted_iota(jnp.int32, (tok, span), 1)
        start = jnp.where(place_ref[0] == 0, WINDOW, 0)
        stop = jnp.where(place_ref[0] == count - 1, tok + WINDOW, span)
        keep = (col >= row) & (col <= row + 2 * WINDOW) & (col >= start) & (col < stop)
        for kv in range(heads // GROUP):
            at = slice(kv * HEAD, (kv + 1) * HEAD)
            k, v = band[:, at], band[:, kc + kv * HEAD : kc + (kv + 1) * HEAD]
            key_sum = value_sum = None
            for h in range(kv * GROUP, (kv + 1) * GROUP):
                cols = slice(h * HEAD, (h + 1) * HEAD)
                q, g = q_ref[:, cols], g_ref[:, cols]
                scores = jnp.where(keep, contract(q, k, 1, 1) * SCALING, MASKED)
                logit = sink_ref[h]
                top = jnp.maximum(jnp.max(scores, axis=-1, keepdims=True), logit)
                raised = jnp.exp(scores - top)
                sink_raised = jnp.exp(logit - top)
                inverse = 1.0 / (jnp.sum(raised, axis=-1, keepdims=True) + sink_raised)
                soft = raised * inverse
                rounded = soft.astype(bf16)
                attended = contract(rounded, v, 1, 0).astype(bf16)
                dots = jnp.sum(
                    g.astype(f32) * attended.astype(f32), axis=-1, keepdims=True
                )
                score_grads = (soft * (contract(g, v, 1, 1) - dots)).astype(bf16)
                both_out[:, cols] = attended
                both_out[:, qc + h * HEAD : qc + (h + 1) * HEAD] = (
                    contract(score_grads, k, 1, 0) * SCALING
                ).astype(bf16)
                key_part = contract(score_grads, q, 0, 0)
                value_part = contract(rounded, g, 0, 0)
                key_sum = key_part if key_sum is None else key_sum + key_part
                value_sum = value_part if value_sum is None else value_sum + value_part
                part = -jnp.sum(sink_raised * inverse * dots, axis=0, keepdims=True)
                sink_out[:, cols] = jnp.broadcast_to(part, (SINK_ROWS, HEAD))
            for base, total in ((0, key_sum * SCALING), (kc, value_sum)):
                cols = slice(base + kv * HEAD, base + (kv + 1) * HEAD)
                low = total[:WINDOW].astype(bf16)
                high = total[WINDOW + tok :].astype(bf16)
                first_out[:, cols] = jnp.where(even, high, low)
                second_out[:, cols] = jnp.where(even, low, high)
                mine_out[:, cols] = total[WINDOW : WINDOW + tok]

    outs = [
        pltpu.VMEM((tok, 2 * qc), bf16),
        pltpu.VMEM((tok, 2 * kc), f32),
        pltpu.VMEM((WINDOW, 2 * kc), bf16),
        pltpu.VMEM((WINDOW, 2 * kc), bf16),
        pltpu.VMEM((SINK_ROWS, qc), f32),
    ]
    return pl.pallas_call(
        body,
        in_specs=[SMEM, SMEM] + [VMEM] * 5,
        out_specs=[VMEM] * 5,
        out_shape=outs,
        cost_estimate=cost(10 * tok * span * qc * 4, 8 * tok * qc),
        name="attention",
        compiler_params=grant(16),
    )(place, sink, *on_chip(queries, grads, own, first, second))


def add_edges(place, mine, first, second, sink_part):
    tok, cols = mine.shape

    def body(place_ref, mine_ref, first_ref, second_ref, sink_ref, out_ref, acc):
        even = place_ref[0] % 2 == 0
        one, other = first_ref[...].astype(f32), second_ref[...].astype(f32)
        acc[...] = mine_ref[...]
        acc[tok - WINDOW :, :] += jnp.where(even, one, other)
        acc[:WINDOW, :] += jnp.where(even, other, one)
        out_ref[:tok, :] = acc[...].astype(bf16)
        row = lax.broadcasted_iota(jnp.int32, (SINK_ROWS, cols), 0)
        left = sink_ref[...]
        pieces = jnp.zeros((SINK_ROWS, cols), f32)
        for n in range(3):
            piece = left.astype(bf16).astype(f32)
            pieces = jnp.where(row == n, piece, pieces)
            left = left - piece
        out_ref[tok:, :] = pieces.astype(bf16)

    return pl.pallas_call(
        body,
        in_specs=[SMEM] + [VMEM] * 4,
        out_specs=VMEM,
        out_shape=pltpu.VMEM((tok + SINK_ROWS, cols), bf16),
        scratch_shapes=[pltpu.VMEM(mine.shape, f32)],
        cost_estimate=cost(tok * cols * 100, 8 * tok * cols),
        name="add_edges",
        compiler_params=grant(4),
    )(place, *on_chip(mine, first, second, sink_part))


def input_parts(place, both, kv_grads, weights):
    qw, kw, _ = weights
    tok = both.shape[0]
    qc, kc = qw.shape[1], kw.shape[1]
    feat = qw.shape[0] // 4

    def body(place_ref, both_ref, kv_ref, qr, kr, vr, sent, kept):
        for out, index, away in ((sent, 0, 1), (sent, 1, 3), (kept, 0, 0), (kept, 1, 2)):
            at = pl.ds(pl.multiple_of((place_ref[1] ^ away) * feat, feat), feat)
            out[index] = (
                contract(qr[at, :], both_ref[:, qc:], 1, 1)
                + contract(kr[at, :], kv_ref[:tok, :kc], 1, 1)
                + contract(vr[at, :], kv_ref[:tok, kc:], 1, 1)
            ).T.astype(bf16)

    out = pltpu.VMEM((2, tok, feat), bf16)
    return pl.pallas_call(
        body,
        in_specs=[SMEM] + [VMEM] * 5,
        out_specs=[VMEM, VMEM],
        out_shape=[out, out],
        cost_estimate=cost(8 * tok * feat * (qc + 2 * kc), 8 * feat * (qc + 2 * kc)),
        compiler_params=grant(10),
        name="input_parts",
    )(place, *on_chip(both, kv_grads, *weights))


def token_block(place_ref, offset, count):
    own = place_ref[0]
    position = jnp.where(own % 2 == 0, own // 2, count - 1 - own // 2) + offset
    position = jnp.where(position < 0, position + count, position)
    position = jnp.where(position >= count, position - count, position)
    return jnp.where(position < count // 2, 2 * position, 2 * (count - 1 - position) + 1)


def side_index(place_ref, block, half, r):
    own, tp = place_ref[0], place_ref[1]
    core = (block // r % 2) ^ (tp % 2)
    far = half ^ (tp // 2)
    step = (block % r) ^ (own % r)
    flip = (block // (2 * r)) ^ (own // (2 * r))
    return ((core * 2 + far) * r + step) * 2 + flip


def ring_offset(n):
    return (n + 1) // 2 * (-1 if n % 2 else 1)


def weights_early(place, sides, boths, kvs, start, sums, count, qc, kc):
    r = count // 4
    half, width = sides.shape[2:]
    tok, blocks = 2 * half, len(boths)
    tokens = blocks * tok

    def body(place_ref, side_ref, *refs):
        both_refs, kv_refs, refs = refs[:blocks], refs[blocks : 2 * blocks], refs[2 * blocks :]
        so_far, refs = refs[: len(sums)], refs[len(sums) :]
        q_out, kv_out, o_out, sink_out, x_all, g_all, both_all, kv_all = refs
        if sums:
            sink_out[...] = so_far[3][...]
        for n in range(blocks):
            block = token_block(place_ref, ring_offset(start + n), count)
            for i in range(2):
                at = side_index(place_ref, block, i, r)
                rows = slice(n * tok + i * half, n * tok + (i + 1) * half)
                x_all[rows, :] = side_ref[at, 0]
                g_all[rows, :] = side_ref[at, 1]
            rows = slice(n * tok, (n + 1) * tok)
            both_all[rows, :] = both_refs[n][...]
            kv_all[rows, :] = kv_refs[n][:tok, :]
            sink_out[block] = kv_refs[n][tok:, :]
        for n, out, left, right in (
            (2, o_out, both_all[:, :qc], g_all[...]),
            (0, q_out, x_all[...], both_all[:, qc:]),
            (1, kv_out, x_all[...], kv_all[...]),
        ):
            value = contract(left, right, 0, 0)
            out[...] = so_far[n][...] + value if sums else value

    return pl.pallas_call(
        body,
        in_specs=[SMEM] + [VMEM] * (2 * blocks + 1 + len(sums)),
        out_specs=[VMEM] * 4,
        out_shape=[
            pltpu.VMEM((width, qc), f32),
            pltpu.VMEM((width, 2 * kc), f32),
            pltpu.VMEM((qc, width), f32),
            pltpu.VMEM((count, SINK_ROWS, 2 * kc), bf16),
        ],
        scratch_shapes=[
            pltpu.VMEM((tokens, width), bf16),
            pltpu.VMEM((tokens, width), bf16),
            pltpu.VMEM((tokens, 2 * qc), bf16),
            pltpu.VMEM((tokens, 2 * kc), bf16),
        ],
        cost_estimate=cost(2 * tokens * width * (2 * qc + 2 * kc), 8 * tokens * width),
        compiler_params=grant(20),
    )(place, *on_chip(sides, *boths, *kvs, *sums))


def weights_late(place, sides, both_halves, kv_halves, sums, sinks, qc, kc):
    count = sinks.shape[0]
    r = count // 4
    half, width = sides.shape[2:]
    tok = 2 * half

    def body(place_ref, side_ref, att, dq, dk, dv, q_in, kv_in, o_in, sink_in,
             q_out, k_out, v_out, o_out, sink_out):
        block = token_block(place_ref, count // 2, count)
        at = [side_index(place_ref, block, i, r) for i in range(2)]
        x = jnp.concatenate([side_ref[i, 0] for i in at], axis=0)
        g = jnp.concatenate([side_ref[i, 1] for i in at], axis=0)
        o_out[...] = o_in[...] + contract(att[...], g, 0, 0)
        q_out[...] = q_in[...] + contract(x, dq[...], 0, 0)
        k_out[...] = kv_in[:, :kc] + contract(x, dk[:tok, :], 0, 0)
        v_out[...] = kv_in[:, kc:] + contract(x, dv[:tok, :], 0, 0)
        last = jnp.concatenate([dk[tok:, :], dv[tok:, :]], axis=1).astype(f32)
        total = None
        for n in range(count):
            rows = jnp.where(block == n, last, sink_in[n].astype(f32))
            value = rows[0:1] + rows[1:2] + rows[2:3]
            total = value if total is None else total + value
        for h in range(qc // HEAD):
            sink_out[h] = jnp.max(total[:, h * HEAD : (h + 1) * HEAD])

    shapes = [(width, qc), (width, kc), (width, kc), (qc, width)]
    return pl.pallas_call(
        body,
        in_specs=[SMEM] + [VMEM] * 9,
        out_specs=[VMEM] * 4 + [SMEM],
        out_shape=[jax.ShapeDtypeStruct(shape, f32) for shape in (*shapes, (qc // HEAD,))],
        cost_estimate=cost(2 * tok * width * (2 * qc + 2 * kc), 16 * width * qc),
        compiler_params=grant(12),
        name="weights_late",
    )(place, *on_chip(sides, *both_halves, *kv_halves, *sums, sinks))


def block_halves(place, own, across):
    tok, feat = own[0].shape
    r = lax.axis_size("sp") // 4
    half, width = tok // 2, feat // r

    def body(place_ref, own_x, own_g, across_x, across_g, *outs):
        high = place_ref[1] // 2
        rows = pl.ds(pl.multiple_of(high * half, half), half)
        same = place_ref[0] // (2 * r) == high

        def cut(sources):
            for n, out in enumerate(outs):
                at = pl.multiple_of(((place_ref[0] % r) ^ (n % r)) * width, width)
                for i, source in enumerate(sources[n // r]):
                    out[i] = source[rows, pl.ds(at, width)]

        here, there = (own_x, own_g), (across_x, across_g)
        pl.when(same)(lambda: cut((here, there)))
        pl.when(jnp.logical_not(same))(lambda: cut((there, here)))

    outs = pl.pallas_call(
        body,
        in_specs=[SMEM] + [VMEM] * 4,
        out_specs=[VMEM] * (2 * r),
        out_shape=[pltpu.VMEM((2, half, width), bf16)] * (2 * r),
        cost_estimate=cost(10**7, 8 * tok * feat),
        compiler_params=grant(2),
        name="block_halves",
    )(place, *on_chip(*own, *across))
    return outs[:r], outs[r:]


def send_half(flip, step, value):
    count = lax.axis_size("sp")
    r = count // 4
    pairs = []
    for a in range(4):
        for b in range(r):
            for j in range(4):
                target = (((a // 2) ^ flip) * 2 + j % 2) * r + (b ^ step)
                pairs.append(((a * r + b) * 4 + j, target * 4 + (j // 2) * 2 + a % 2))
    return lax.ppermute(value, ("sp", "tp"), pairs)


def stack_near(pieces):
    def body(*refs):
        for n, ref in enumerate(refs[:-1]):
            refs[-1][n] = ref[...]

    return pl.pallas_call(
        body,
        in_specs=[VMEM] * len(pieces),
        out_specs=VMEM,
        out_shape=pltpu.VMEM((len(pieces), *pieces[0].shape), bf16),
        cost_estimate=cost(10**7, 2**21),
        compiler_params=grant(2),
        name="stack_near",
    )(*on_chip(*pieces))


def spread_slices(near):
    near = stack_near(near)
    far = swap_tp(near, 2)
    sides = jnp.stack([near, far, swap_tp(near, 1), swap_tp(far, 1)])
    return sides.reshape(-1, *near.shape[1:])


def gathers_operands(count, tok, depth, qc, kc):
    gathered = count * tok * (2 * depth // count + 2 * qc + 2 * kc) * 2
    return (
        gathered < depth * (2 * qc + 2 * kc) * 4
        and (depth // count) % 128 == 0
        and count % 4 == 0
        and qc == 2 * kc
    )


def layer_backward(
    layer_input, output_grad, query_weight, key_weight, value_weight, out_weight, sink_logit
):
    count = lax.axis_size("sp")
    qc, kc = query_weight.shape[1], key_weight.shape[1]
    tok = layer_input.shape[0]
    depth = query_weight.shape[0]
    tp, sp = lax.axis_index("tp"), lax.axis_index("sp")
    place = jnp.stack([sp, tp])
    gathers = gathers_operands(count, tok, depth, qc, kc)

    x_y, g_y = swap_tp(layer_input, 2), swap_tp(output_grad, 2)
    x_c, g_c = swap_tp(layer_input, 1), swap_tp(output_grad, 1)
    own_x, own_g, *rows_weights, out_weight = stage(
        layer_input, output_grad, query_weight, key_weight, value_weight, out_weight
    )
    if gathers:
        stay, leave = block_halves(place, (own_x, own_g), (x_y, g_y))
        near = []
        for step in range(count // 4):
            near += [send_half(0, step, stay[step]), send_half(1, step, leave[step])]
    x_yc, g_yc = swap_tp(x_y, 1), swap_tp(g_y, 1)
    row_sums = rows_part(place, (own_x, x_c), 0, (), rows_weights, False)
    queries, key_values, first, second = rows_part(place, (x_y, x_yc), 2, row_sums, rows_weights, True)
    first, second = swap_sp(first, 0), swap_sp(second, 1)
    grad_sum = grad_part(place, (own_g, g_c), 0, (), out_weight, False)
    grads = grad_part(place, (g_y, g_yc), 2, (grad_sum,), out_weight, True)

    both, mine, first, second, sink_part = attention(
        place, sink_logit, queries, grads, key_values, first, second
    )
    first, second = swap_sp(first, 0), swap_sp(second, 1)
    kv_grads = add_edges(place, mine, first, second, sink_part)

    sent, kept = input_parts(place, both, kv_grads, rows_weights)
    kept = (kept.astype(f32) + swap_tp(sent, 1).astype(f32)).astype(bf16)
    from_far = swap_tp(kept[1], 2)
    input_grad = (kept[0].astype(f32) + from_far.astype(f32)).astype(bf16)

    if gathers:
        sides = spread_slices(near)
        boths, kvs = ring_gather(both), ring_gather(kv_grads)
        sums = ()
        for first, stop in ((0, count - 3), (count - 3, count - 1)):
            sums = weights_early(
                place, sides, boths[first:stop], kvs[first:stop], first, sums, count, qc, kc
            )
        *sums, sinks = sums
        q_part, k_part, v_part, o_part, sink_grad = weights_late(
            place, sides, boths[-2:], kvs[-2:], sums, sinks, qc, kc
        )
    else:
        blocks = lambda *parts: jnp.concatenate(
            [lax.dynamic_index_in_dim(jnp.stack(parts), tp ^ i, keepdims=False)
             for i in range(4)], axis=1)
        whole_input = blocks(layer_input, x_c, x_y, x_yc)
        whole_grad = blocks(output_grad, g_c, g_y, g_yc)
        sums = jnp.concatenate(
            [
                contract(whole_input, both[:, qc:], 0, 0),
                contract(whole_grad, both[:, :qc], 0, 0),
                contract(whole_input, kv_grads[:tok], 0, 0),
            ],
            axis=1,
        )
        sums = lax.psum_scatter(sums, "sp", scatter_dimension=0, tiled=True)
        q_part, o_part = sums[:, :qc], sums[:, qc : 2 * qc].T
        k_part = sums[:, 2 * qc : 2 * qc + kc]
        v_part = sums[:, 2 * qc + kc :]
        sink_grad = lax.psum(sink_part[0, ::HEAD], "sp")
    return (input_grad, q_part, k_part, v_part, o_part, sink_grad)


def solution(mesh):
    placed = (
        P("sp", "tp"),
        P("sp", "tp"),
        P(None, "tp"),
        P(None, "tp"),
        P(None, "tp"),
        P("tp", None),
        P("tp"),
    )
    return jax.shard_map(
        layer_backward,
        mesh=mesh,
        in_specs=placed,
        out_specs=(
            P("sp", "tp"),
            P("sp", "tp"),
            P("sp", "tp"),
            P("sp", "tp"),
            P("tp", "sp"),
            P("tp"),
        ),
        check_vma=False,
    )
```
